32 devices in a mesh: sp: 16 (over z, y, x), tp: 2 (over core).
Axes of the slice: x: 2, y: 2, z: 4, core: 2. Of those that a mesh axis runs over, the one named last changes fastest.
Arguments:
- residual: bfloat16 [4096, 2048], P(('sp', 'tp')), may hold values from -6 to 6
- queries: bfloat16 [4096, 1024], P('sp', 'tp'), may hold values from -6 to 6
- keys: bfloat16 [4096, 1024], P('sp', 'tp'), may hold values from -6 to 6
- values: bfloat16 [4096, 2048], P('sp', 'tp'), may hold values from -6 to 6
- out_gate: bfloat16 [4096, 2048], P('sp', 'tp'), may hold values from -6 to 6
- in_gate: float32 [2, 4096, 8], P(None, 'sp', 'tp'), may hold values from -6 to 140, as said below
- forget_gate: float32 [2, 4096, 8], P(None, 'sp', 'tp'), may hold values from 0 to 20
- head_gain: float32 [2048], P('tp'), may hold values from 0.1 to 1.9
- w_out: bfloat16 [2048, 2048], P('tp'), may hold values from -0.125 to 0.125
- norm_gain: float32 [2048], replicated, may hold values from 0.1 to 1.9
- shared_gate: bfloat16 [2048, 512], replicated, may hold values from -0.125 to 0.125
- shared_up: bfloat16 [2048, 512], replicated, may hold values from -0.125 to 0.125
- shared_down: bfloat16 [512, 2048], replicated, may hold values from -0.25 to 0.25
- w_gate: bfloat16 [32, 2048, 512], P(('sp', 'tp')), may hold values from -0.125 to 0.125
- w_up: bfloat16 [32, 2048, 512], P(('sp', 'tp')), may hold values from -0.125 to 0.125
- w_down: bfloat16 [32, 512, 2048], P(('sp', 'tp')), may hold values from -0.25 to 0.25
- routes: int32 [4096, 4], P(('sp', 'tp')), may hold values from 0 to 31, all different within a row; in each aligned block of 128 rows (0 to 127, 128 to 255, ...) at most 32 rows name the same one
- route_weight: float32 [4096, 4], P(('sp', 'tp')), may hold values from 0.3 to 1.5
Outputs:
- layer_out: bfloat16 [4096, 2048], P(('sp', 'tp'))
The draws below stay inside these ranges and needn't reach their ends.
Inputs may be any that keep to these rules, and one draw needn't show every extreme that they name: `in_gate`: log input gates mostly of order one. `routes`: each row names 4 different experts. Among the rows of one device (aligned blocks of 128 rows) no expert is named more than 32 times, a bound that some block reaches.
All inputs are finite; a program needn't handle non-finite values.
Results may differ from the reference program's by a relative error of at most 0.017.
Values may be sent and summed in bfloat16 or wider, within the bound.
No kernel may reach another device: no remote copies, remote signals or barrier semaphores. Data moves between devices by JAX's collectives and lax.ppermute only.
A program may use at most 128 MiB of HBM per device.

```python
import math
import jax
import jax.numpy as jnp
import numpy as np
from jax import lax

D = 2048
MEMORY_SPLITS = 8
DQK = 128
DV = 256
EXPERT_FF = 512
SHARED_FF = 512
TOP_K = 4
TOK_DEV = 256
TOK_HALF = 128
TOKENS = 4096
EXPERTS = 32
CAP = 32


def draw_in_gate(key, part):
    lookup_series = jax.random.split(key, 1)
    shape = (2, TOKENS, MEMORY_SPLITS)
    switch_levels = jnp.clip(jax.random.normal(lookup_series[0], shape, jnp.float32), -6.0, 6.0)
    return switch_levels.astype(jnp.float32)


def draw_forget_gate(key, part):
    lookup_series = jax.random.split(key, 5)
    shape = (2, TOKENS, MEMORY_SPLITS)
    fast_heads = jax.random.bernoulli(lookup_series[0], 0.5, (2, 1, MEMORY_SPLITS))
    noise = jnp.clip(jax.random.normal(lookup_series[2], shape, jnp.float32) * 0.8, -2.4, 2.4)
    level = jnp.where(fast_heads, math.log(40.0), math.log(TOKENS) + 1.1)
    block_count = TOKENS // TOK_DEV
    shift = jnp.repeat(jax.random.uniform(lookup_series[1], (2, block_count, MEMORY_SPLITS), jnp.float32, -0.7, 0.7), TOK_DEV, axis=1)
    switch_levels = level + shift + noise
    bucket_indices = jax.random.randint(lookup_series[3], (2, 3), 0, TOKENS)
    packet_bundles = jax.random.uniform(lookup_series[4], (2, 3, MEMORY_SPLITS), jnp.float32, 0.0, 1.4)
    sweep_heading = jnp.arange(2)[:, None]
    switch_levels = switch_levels.at[sweep_heading, bucket_indices].set(packet_bundles)
    return jnp.clip(switch_levels, 0.0, 20.0).astype(jnp.float32)


def block_scale(key, extent, cuts, least, top_value):
    def one(axis_at, shards_of):
        steps = jax.random.uniform(jax.random.fold_in(jax.random.fold_in(key, 6), axis_at), (shards_of,), jnp.float32, least / len(cuts), top_value / len(cuts))
        return jnp.repeat(jnp.exp(steps), extent[axis_at] // shards_of).reshape((-1,) + (1,) * (len(extent) - axis_at - 1))

    factor_of = one(*cuts[0])
    for cut in cuts[1:]:
        factor_of = factor_of * one(*cut)
    return factor_of


def routed_block(rng, own, number, rows, count, top, bound, skew):
    order = jax.random.permutation(rng, count)
    packed, usual = shares(count, rows * top, bound, skew, True), shares(count, rows * top, bound, skew, False)
    places = jnp.arange(count)

    def named(tallies, offset_by):
        used = int((tallies > 0).sum())
        fixed = max(1, used // 4)
        shifted = fixed + (places - fixed + offset_by * (used - fixed)) % max(1, count - fixed)
        return jnp.zeros((count,), jnp.int32).at[order[jnp.where(places < fixed, places, shifted)]].set(jnp.asarray(tallies, jnp.int32))

    tallies = jnp.where(number % 4 == 0, named(packed, number // 4), named(usual, number - number // 4 - 1))
    mixed = jax.random.permutation(jax.random.fold_in(own, 3), count)
    donor, receiver = mixed[0:count // 2 * 2:2], mixed[1:count // 2 * 2:2]
    slack = jnp.minimum(tallies[donor] - 1, bound - tallies[receiver]) // 2
    slack = jnp.where((donor == order[0]) | (receiver == order[0]) | (tallies[receiver] == 0), 0, jnp.maximum(slack, 0))
    shifted = jax.random.randint(jax.random.fold_in(own, 4), (count // 2,), 0, 1 << 20) % (slack + 1)
    tallies = tallies.at[donor].add(-shifted).at[receiver].add(shifted)
    items = jnp.searchsorted(jnp.cumsum(tallies), jnp.arange(rows * top), side="right").astype(jnp.int32)
    table = items.reshape(top, rows).T
    table = table[jax.random.permutation(jax.random.fold_in(own, 1), rows)]
    offset_by = jax.random.randint(jax.random.fold_in(own, 2), (rows, 1), 0, top)
    return jnp.take_along_axis(table, (jnp.arange(top)[None, :] + offset_by) % top, axis=1)


def shares(amount, total, most, skew, full):
    loads = [(1 << 20) // math.isqrt(standing ** skew) + 1 for standing in range(1, amount + 1)]
    largest = most if full else min(most, max(-(-total // amount), total * loads[0] // sum(loads)))
    least = 1 if total - largest >= amount - 1 else 0
    holding, surplus = [largest] + [least] * (amount - 1), total - largest - least * (amount - 1)
    while surplus > 0:
        free = [i for i in range(1, amount) if holding[i] < largest] or [i for i in range(1, amount) if holding[i] < most]
        pool, budget = sum([loads[i] for i in free]), surplus
        for i in free:
            extra = min(most - holding[i], max(1, budget * loads[i] // pool), surplus)
            holding[i] = holding[i] + extra
            surplus = surplus - extra
    return np.array(holding)


def centred(own_key, shape, scale, bound, cuts=(), held_as=jnp.bfloat16):
    loudness = block_scale(own_key, shape, cuts, -0.22, 0.18) if cuts else 1.0
    array = jax.random.normal(own_key, shape, jnp.float32) * scale * loudness
    return jnp.minimum(jnp.maximum(array, -bound), bound).astype(held_as)


def setup_inputs(seed: int = 0) -> dict:
    key_of = jax.random.split(jax.random.key(seed), 19)
    residual = centred(key_of[0], (TOKENS, D), 1.0, 6.0, ((0, 32),))
    queries = centred(key_of[1], (TOKENS, MEMORY_SPLITS * DQK), 1.0, 6.0, ((0, 16), (1, 2)))
    keys = centred(key_of[2], (TOKENS, MEMORY_SPLITS * DQK), 1.0, 6.0, ((0, 16), (1, 2)))
    values = centred(key_of[3], (TOKENS, MEMORY_SPLITS * DV), 1.0, 6.0, ((0, 16), (1, 2)))
    out_gate = centred(key_of[4], (TOKENS, MEMORY_SPLITS * DV), 1.5, 6.0, ((0, 16), (1, 2)))
    in_gate = draw_in_gate(jax.random.fold_in(key_of[18], 71), 0)
    forget_gate = draw_forget_gate(jax.random.fold_in(key_of[18], 71), 0)
    head_gain = jnp.clip(1.0 + 0.18 * jax.random.normal(key_of[7], (MEMORY_SPLITS * DV,), jnp.float32), 0.1, 1.9)
    w_out = centred(key_of[8], (MEMORY_SPLITS * DV, D), (MEMORY_SPLITS * DV) ** -0.5, 0.125, ((0, 2),))
    norm_gain = jnp.clip(1.0 + 0.18 * jax.random.normal(key_of[9], (D,), jnp.float32), 0.1, 1.9)
    shared_gate = centred(key_of[10], (D, SHARED_FF), D ** -0.5, 0.125)
    shared_up = centred(key_of[11], (D, SHARED_FF), D ** -0.5, 0.125)
    shared_down = centred(key_of[12], (SHARED_FF, D), SHARED_FF ** -0.5, 0.25)
    w_gate = centred(key_of[13], (EXPERTS, D, EXPERT_FF), D ** -0.5, 0.125, ((0, 32),))
    w_up = centred(key_of[14], (EXPERTS, D, EXPERT_FF), D ** -0.5, 0.125, ((0, 32),))
    w_down = centred(key_of[15], (EXPERTS, EXPERT_FF, D), EXPERT_FF ** -0.5, 0.25, ((0, 32),))
    routes_keys = jax.random.split(jax.random.fold_in(key_of[16], 1), TOKENS // TOK_HALF)
    routes_turns = jax.random.permutation(jax.random.fold_in(key_of[16], 3), TOKENS // TOK_HALF)
    routes = jax.vmap(lambda own, number: routed_block(jax.random.fold_in(key_of[16], 2), own, number, TOK_HALF, EXPERTS, TOP_K, CAP, 2))(routes_keys, routes_turns).reshape((TOKENS, TOP_K))
    route_weight = jnp.clip(jnp.exp(math.log(1.5) - 1.60943787 * jax.random.uniform(key_of[17], (TOKENS, TOP_K), jnp.float32) ** block_scale(key_of[17], (TOKENS, TOP_K), ((0, 32),), -0.2, 0.2)), 0.3, 1.5)
    return {"residual": residual, "queries": queries, "keys": keys, "values": values, "out_gate": out_gate, "in_gate": in_gate, "forget_gate": forget_gate, "head_gain": head_gain, "w_out": w_out, "norm_gain": norm_gain, "shared_gate": shared_gate, "shared_up": shared_up, "shared_down": shared_down, "w_gate": w_gate, "w_up": w_up, "w_down": w_down, "routes": routes, "route_weight": route_weight}


epsilon = 1e-06
max_floor = -1e+30
block_rows = 128

def direction_pass(query_heads, key_heads, value_heads, gate_input, log_forget, block_len):
    seq_len, head_count, key_dim = key_heads.shape
    value_dim = value_heads.shape[2]
    block_count = seq_len // block_len
    key_scale = 1.0 / math.sqrt(key_dim)
    pieces_all = (query_heads.reshape(block_count, block_len, head_count, key_dim), key_heads.reshape(block_count, block_len, head_count, key_dim), value_heads.reshape(block_count, block_len, head_count, value_dim), gate_input.reshape(block_count, block_len, head_count), log_forget.reshape(block_count, block_len, head_count))
    lower = jnp.tril(jnp.ones((block_len, block_len), dtype=bool))

    def block_step(carry, pieces):
        state_matrix, state_norm, state_max = carry
        block_query, block_key, block_value, block_in, block_forget = pieces
        running = jnp.cumsum(block_forget, axis=0)
        block_decay = running[-1]
        log_weight = block_decay[None, :] - running + block_in
        block_max = lax.optimization_barrier(jnp.max(log_weight, axis=0))
        scaled = jnp.exp(log_weight - block_max[None, :]) * key_scale
        weighted_low = lax.optimization_barrier((block_key.astype(jnp.float32) * scaled[:, :, None]).astype(jnp.bfloat16))
        weighted_keys = weighted_low.astype(jnp.float32)
        value_wide = block_value.astype(jnp.float32)
        query_wide = block_query.astype(jnp.float32)
        block_matrix = jnp.einsum('thd,the->hde', weighted_keys, value_wide)
        block_norm = lax.optimization_barrier(jnp.sum(weighted_keys, axis=0))
        running_heads = running.T
        pair_log = running_heads[:, :, None] - running_heads[:, None, :] + block_in.T[:, None, :]
        pair_log = jnp.where(lower[None], pair_log, -jnp.inf)
        crossing_peak = running_heads + state_max[:, None]
        row_max = jnp.maximum(crossing_peak, lax.optimization_barrier(jnp.max(pair_log, axis=2)))
        scores = jnp.einsum('thd,shd->hts', query_wide, block_key.astype(jnp.float32)) * key_scale
        cell_weight = jnp.exp(pair_log - row_max[:, :, None]) * scores
        weight_low = lax.optimization_barrier(cell_weight.astype(jnp.bfloat16)).astype(jnp.float32)
        inter_scale = jnp.exp(crossing_peak - row_max)
        read_state = jnp.einsum('thd,hde->hte', query_wide, state_matrix, precision=lax.Precision.HIGHEST)
        read_norm = jnp.einsum('thd,hd->ht', query_wide, state_norm, precision=lax.Precision.HIGHEST)
        numerator = inter_scale[:, :, None] * read_state + jnp.einsum('hts,she->hte', weight_low, value_wide)
        denominator = inter_scale * read_norm + lax.optimization_barrier(jnp.sum(cell_weight, axis=2))
        result = numerator / jnp.maximum(jnp.abs(denominator), jnp.exp(-row_max))[:, :, None]
        new_max = jnp.maximum(block_decay + state_max, block_max)
        keep_scale = jnp.exp(block_decay + state_max - new_max)
        add_scale = jnp.exp(block_max - new_max)
        new_matrix = keep_scale[:, None, None] * state_matrix + add_scale[:, None, None] * block_matrix
        new_norm = keep_scale[:, None] * state_norm + add_scale[:, None] * block_norm
        return ((new_matrix, new_norm, new_max), jnp.transpose(result, (1, 0, 2)))
    start_state = (jnp.zeros((head_count, key_dim, value_dim), jnp.float32), jnp.zeros((head_count, key_dim), jnp.float32), jnp.full((head_count,), max_floor, jnp.float32))
    _, results = lax.scan(block_step, start_state, pieces_all)
    return results.reshape(seq_len, head_count, value_dim)

def routed_experts(normed, w_gate, w_up, w_down, routes, route_weight):
    token_count, model_width = normed.shape
    expert_count = w_gate.shape[0]
    top_count = routes.shape[1]
    assign_count = token_count * top_count
    flat_expert = routes.reshape(assign_count).astype(jnp.int32)
    order = jnp.argsort(flat_expert, stable=True).astype(jnp.int32)
    sorted_expert = flat_expert[order]
    counts = jnp.zeros((expert_count,), jnp.int32).at[flat_expert].add(1)
    padded = ((counts + block_rows - 1) // block_rows * block_rows).astype(jnp.int32)
    pad_end = jnp.cumsum(padded).astype(jnp.int32)
    pad_start = (pad_end - padded).astype(jnp.int32)
    first_of = (jnp.cumsum(counts).astype(jnp.int32) - counts).astype(jnp.int32)
    destination = (pad_start[sorted_expert] + jnp.arange(assign_count, dtype=jnp.int32) - first_of[sorted_expert]).astype(jnp.int32)
    slot_total = (assign_count + expert_count * (block_rows - 1) + block_rows - 1) // block_rows * block_rows
    block_total = slot_total // block_rows
    flat_token = jnp.arange(assign_count, dtype=jnp.int32) // top_count
    slot_token = jnp.zeros((slot_total,), jnp.int32).at[destination].set(flat_token[order])
    block_expert = jnp.minimum(jnp.searchsorted(pad_end, jnp.arange(block_total, dtype=jnp.int32) * block_rows, side='right'), expert_count - 1).astype(jnp.int32)
    block_inputs = normed[slot_token].reshape(block_total, block_rows, model_width)

    def one_block(operands):
        block_input, expert_id = operands
        gate_part = jnp.dot(block_input, w_gate[expert_id], preferred_element_type=jnp.float32)
        up_part = jnp.dot(block_input, w_up[expert_id], preferred_element_type=jnp.float32)
        hidden = (jax.nn.silu(gate_part) * up_part).astype(jnp.bfloat16)
        return jnp.dot(hidden, w_down[expert_id], preferred_element_type=jnp.float32).astype(jnp.bfloat16)
    block_outputs = lax.map(one_block, (block_inputs, block_expert)).reshape(slot_total, model_width)
    sorted_outputs = block_outputs[destination]
    assigned = jnp.zeros((assign_count, model_width), jnp.bfloat16).at[order].set(sorted_outputs)
    weighted = assigned.astype(jnp.float32).reshape(token_count, top_count, model_width) * route_weight[:, :, None]
    return lax.optimization_barrier(jnp.sum(weighted, axis=1))

def reference(residual, queries, keys, values, out_gate, in_gate, forget_gate, head_gain, w_out, norm_gain, shared_gate, shared_up, shared_down, w_gate, w_up, w_down, routes, route_weight):
    query_heads = queries.reshape(TOKENS, MEMORY_SPLITS, DQK)
    key_heads = keys.reshape(TOKENS, MEMORY_SPLITS, DQK)
    value_heads = values.reshape(TOKENS, MEMORY_SPLITS, DV)
    log_forget = jax.nn.log_sigmoid(forget_gate)
    forward_out = direction_pass(query_heads, key_heads, value_heads, in_gate[0], log_forget[0], TOK_DEV)
    backward_out = direction_pass(query_heads[::-1], key_heads[::-1], value_heads[::-1], in_gate[1][::-1], log_forget[1][::-1], TOK_DEV)[::-1]
    summed = forward_out + backward_out
    normal = summed * lax.rsqrt(lax.optimization_barrier(jnp.mean(summed * summed, axis=-1, keepdims=True)) + epsilon)
    mixed_heads = (normal.reshape(TOKENS, MEMORY_SPLITS * DV) * head_gain * jax.nn.sigmoid(out_gate.astype(jnp.float32))).astype(jnp.bfloat16)
    projected = jnp.dot(mixed_heads, w_out, preferred_element_type=jnp.float32)
    updated = (residual.astype(jnp.float32) + projected).astype(jnp.bfloat16)
    updated_wide = updated.astype(jnp.float32)
    normed = (updated_wide * lax.rsqrt(lax.optimization_barrier(jnp.mean(updated_wide * updated_wide, axis=-1, keepdims=True)) + epsilon) * norm_gain).astype(jnp.bfloat16)
    shared_expert_hidden = (jax.nn.silu(jnp.dot(normed, shared_gate, preferred_element_type=jnp.float32)) * jnp.dot(normed, shared_up, preferred_element_type=jnp.float32)).astype(jnp.bfloat16)
    shared = jnp.dot(shared_expert_hidden, shared_down, preferred_element_type=jnp.float32)
    routed = routed_experts(normed, w_gate, w_up, w_down, routes, route_weight)
    return (updated_wide + shared + routed).astype(jnp.bfloat16)
```

```python
import functools
import math

import jax
import jax.numpy as jnp
from jax import lax
from jax.experimental import pallas as pl
from jax.experimental.pallas import tpu as pltpu
from jax.sharding import PartitionSpec as P

epsilon = 1e-06
max_floor = -1e30
stat_rows = 16
f32 = jnp.float32
bf16 = jnp.bfloat16


def three_parts(wide):
    high = wide.astype(bf16).astype(f32)
    rest = wide - high
    middle = rest.astype(bf16).astype(f32)
    return (high, middle, rest - middle)


def pack_stats(norm, first, second):
    row = lax.broadcasted_iota(jnp.int32, (stat_rows, norm.shape[1]), 0)
    left = jnp.zeros(row.shape, f32)
    right = jnp.zeros(row.shape, f32)
    for at, part in enumerate(three_parts(norm)):
        left = jnp.where(row == at, part, left)
    for at, part in enumerate(three_parts(first) + three_parts(second)):
        right = jnp.where(row == at, part, right)
    return jnp.concatenate([left, right], axis=1).astype(bf16)


def sum_parts(tile, start, low, high):
    wide = tile[start : start + 3, low:high]
    return wide[0:1] + wide[1:2] + wide[2:3]


def triangles(rows):
    row = lax.broadcasted_iota(jnp.int32, (rows, rows), 0)
    column = lax.broadcasted_iota(jnp.int32, (rows, rows), 1)
    return (column <= row, column >= row)


def exact_dot(a, b):
    return lax.dot_general(
        a, b, (((1,), (0,)), ((), ())), precision=lax.Precision.HIGHEST, preferred_element_type=f32
    )


def running_columns(forget, heads):
    lower, upper = triangles(forget.shape[0])
    column = lax.broadcasted_iota(jnp.int32, forget.shape, 1)
    return jnp.where(
        column < heads,
        exact_dot(lower.astype(f32), forget),
        exact_dot(upper.astype(f32), forget),
    )


def summary_kernel(forget, gate, keys, values, out, *, heads, key_dim, value_dim, piece):
    rows = keys.shape[0]
    running = running_columns(forget[...], heads)
    column = lax.broadcasted_iota(jnp.int32, (1, 2 * heads), 1)
    total = jnp.where(column < heads, running[rows - 1 : rows], running[0:1])
    log_weight = total - running + gate[...]
    block_max = jnp.max(log_weight, axis=0, keepdims=True)
    scaled = jnp.exp(log_weight - block_max) * (1.0 / math.sqrt(key_dim))
    for pair in range(2 * heads):
        h = pair % heads
        key = keys[:, h * key_dim : (h + 1) * key_dim].astype(f32)
        weighted = (key * scaled[:, pair : pair + 1]).astype(bf16)
        matrix = lax.dot_general(
            weighted,
            values[:, h * value_dim : (h + 1) * value_dim],
            (((0,), (0,)), ((), ())),
            preferred_element_type=f32,
        ).astype(bf16)
        norm = jnp.sum(weighted.astype(f32), axis=0, keepdims=True)
        wide = (1, key_dim)
        tile = pack_stats(
            norm,
            jnp.broadcast_to(block_max[:, pair : pair + 1], wide),
            jnp.broadcast_to(total[:, pair : pair + 1], wide),
        )
        count = key_dim // piece
        for s in range(count):
            out[pair * count + s, 0:piece, :] = matrix[s * piece : (s + 1) * piece]
            out[pair * count + s, piece : piece + stat_rows, :] = tile


def prefix_kernel(backward, blocks, out, *, piece, key_dim):
    count = blocks.shape[0]
    width = blocks.shape[2]

    def step(k, before):
        matrix, norm, peak = before
        at = jnp.where(backward[0] != 0, count - 1 - k, k)
        out[at, 0:piece, :] = matrix.astype(bf16)
        out[at, piece : piece + stat_rows, :] = pack_stats(norm, peak, peak)
        tile = blocks[at, piece : piece + stat_rows, :].astype(f32)
        block_norm = sum_parts(tile, 0, 0, key_dim)
        block_max = sum_parts(tile, 0, key_dim, width)
        total = sum_parts(tile, 3, key_dim, width)
        joined = jnp.maximum(total + peak, block_max)
        keep = jnp.exp(total + peak - joined)
        add = jnp.exp(block_max - joined)
        wide_keep = jnp.concatenate([keep] * (width // key_dim), axis=1)
        wide_add = jnp.concatenate([add] * (width // key_dim), axis=1)
        matrix = wide_keep * matrix + wide_add * blocks[at, 0:piece, :].astype(f32)
        return (matrix, keep * norm + add * block_norm, joined)

    lax.fori_loop(
        0,
        count,
        step,
        (
            jnp.zeros((piece, width), f32),
            jnp.zeros((1, key_dim), f32),
            jnp.full((1, key_dim), max_floor, f32),
        ),
    )


def cell_kernel(
    forget, gate, forget_row, gate_row, queries, keys, values, out_gate, gain, states, out,
    *, heads, key_dim, value_dim, piece,
):
    rows = keys.shape[0]
    key_scale = 1.0 / math.sqrt(key_dim)
    running = running_columns(forget[...], heads)
    lower, upper = triangles(rows)
    side = lax.broadcasted_iota(jnp.int32, (2 * heads, rows), 0)
    running_row = jnp.where(
        side < heads,
        exact_dot(forget_row[...], upper.astype(f32)),
        exact_dot(forget_row[...], lower.astype(f32)),
    )
    source = gate_row[...] - running_row
    count = key_dim // piece
    for h in range(heads):
        query = queries[:, h * key_dim : (h + 1) * key_dim]
        value = values[:, h * value_dim : (h + 1) * value_dim]
        scores = lax.dot_general(
            query,
            keys[:, h * key_dim : (h + 1) * key_dim],
            (((1,), (1,)), ((), ())),
            preferred_element_type=f32,
        ) * key_scale
        summed = None
        for direction in range(2):
            pair = direction * heads + h
            tile = states[pair * count, piece : piece + stat_rows, :].astype(f32)
            norm = sum_parts(tile, 0, 0, key_dim)
            peak = sum_parts(tile, 0, key_dim, 2 * key_dim)[:, 0:1]
            matrix = jnp.concatenate(
                [states[pair * count + s, 0:piece, :] for s in range(count)], axis=0
            )
            here = running[:, pair : pair + 1]
            pair_log = jnp.where(
                upper if direction else lower, here + source[pair : pair + 1, :], -jnp.inf
            )
            crossing = here + peak
            row_max = jnp.maximum(crossing, jnp.max(pair_log, axis=1, keepdims=True))
            weight = jnp.exp(pair_log - row_max) * scores
            carry = jnp.exp(crossing - row_max)
            read_state = jnp.dot(query, matrix, preferred_element_type=f32)
            read_norm = jnp.sum(query.astype(f32) * norm, axis=1, keepdims=True)
            local_part = jnp.dot(weight.astype(bf16), value, preferred_element_type=f32)
            divisor = carry * read_norm + jnp.sum(weight, axis=1, keepdims=True)
            divisor = jnp.maximum(jnp.abs(divisor), jnp.exp(-row_max))
            result = (carry * read_state + local_part) / divisor
            summed = result if summed is None else summed + result
        normal = summed * lax.rsqrt(jnp.mean(summed * summed, axis=1, keepdims=True) + epsilon)
        columns = slice(h * value_dim, (h + 1) * value_dim)
        out[:, columns] = (
            normal * gain[:, columns] * jax.nn.sigmoid(out_gate[:, columns].astype(f32))
        ).astype(bf16)


def mixer(queries, keys, values, out_gate, in_gate, forget_gate, head_gain):
    rows = queries.shape[0]
    heads = in_gate.shape[2]
    key_dim = queries.shape[1] // heads
    value_dim = values.shape[1] // heads
    count = lax.axis_size("sp")
    piece = 2 * heads * key_dim // count
    log_forget = jax.nn.log_sigmoid(forget_gate)
    forget = jnp.transpose(log_forget, (1, 0, 2)).reshape(rows, 2 * heads)
    gate = jnp.transpose(in_gate, (1, 0, 2)).reshape(rows, 2 * heads)
    forget_row = jnp.transpose(log_forget, (0, 2, 1)).reshape(2 * heads, rows)
    gate_row = jnp.transpose(in_gate, (0, 2, 1)).reshape(2 * heads, rows)
    sizes = dict(heads=heads, key_dim=key_dim, value_dim=value_dim, piece=piece)
    shape = jax.ShapeDtypeStruct((count, piece + stat_rows, value_dim), bf16)
    in_vmem = pl.BlockSpec(memory_space=pltpu.VMEM)
    summary = pl.pallas_call(
        functools.partial(summary_kernel, **sizes), out_shape=shape, name="summary"
    )(forget, gate, keys, values)
    blocks = lax.all_to_all(summary, "sp", split_axis=0, concat_axis=0, tiled=True)
    backward = (lax.axis_index("sp") * piece // key_dim >= heads).astype(jnp.int32).reshape(1)
    entering = pl.pallas_call(
        functools.partial(prefix_kernel, piece=piece, key_dim=key_dim),
        out_shape=shape,
        in_specs=[pl.BlockSpec(memory_space=pltpu.SMEM), in_vmem],
        name="prefix",
    )(backward, blocks)
    states = lax.all_to_all(entering, "sp", split_axis=0, concat_axis=0, tiled=True)
    return pl.pallas_call(
        functools.partial(cell_kernel, **sizes),
        out_shape=jax.ShapeDtypeStruct(values.shape, bf16),
        name="cell",
    )(
        forget, gate, forget_row, gate_row, queries, keys, values, out_gate,
        head_gain.reshape(1, -1), states,
    )


def routing(routes, route_weight, expert_count, capacity):
    rows = routes.shape[0]
    slots = expert_count * capacity
    named = routes[:, :, None] == jnp.arange(expert_count, dtype=jnp.int32)
    member = jnp.any(named, axis=1).astype(bf16)
    weight = jnp.sum(jnp.where(named, route_weight[:, :, None], 0.0), axis=1)
    row = lax.broadcasted_iota(jnp.int32, (rows, rows), 0)
    column = lax.broadcasted_iota(jnp.int32, (rows, rows), 1)
    rank = jnp.dot((column < row).astype(bf16), member, preferred_element_type=f32)
    expert = lax.broadcasted_iota(jnp.int32, (expert_count, slots), 0)
    slot = lax.broadcasted_iota(jnp.int32, (expert_count, slots), 1)
    spread = slot // capacity == expert
    wide = functools.partial(jnp.dot, preferred_element_type=f32)
    rank_key = jnp.where(member > 0, rank, float(rows)).astype(bf16)
    place = (jnp.arange(slots, dtype=jnp.int32) % capacity).astype(f32)
    hit = wide(rank_key, spread.astype(bf16)) == place
    weights = lax.dot_general(
        weight, spread.astype(f32), (((1,), (0,)), ((), ())),
        precision=lax.Precision.HIGHEST, preferred_element_type=f32,
    )
    weights = jnp.where(hit, weights, 0.0)
    return hit.astype(bf16), weights


def two_parts(weights):
    high = lax.reduce_precision(weights, 8, 7)
    return high.astype(bf16), (weights - high).astype(bf16)


def expert_layer(rows_in, gate_matrix, up_matrix, down_matrix):
    hidden = (
        jax.nn.silu(jnp.dot(rows_in, gate_matrix, preferred_element_type=f32))
        * jnp.dot(rows_in, up_matrix, preferred_element_type=f32)
    ).astype(bf16)
    return jnp.dot(hidden, down_matrix, preferred_element_type=f32)


def local(
    residual,
    queries,
    keys,
    values,
    out_gate,
    in_gate,
    forget_gate,
    head_gain,
    w_out,
    norm_gain,
    shared_gate,
    shared_up,
    shared_down,
    w_gate,
    w_up,
    w_down,
    routes,
    route_weight,
):
    own_rows, model_width = residual.shape
    mixed_heads = mixer(queries, keys, values, out_gate, in_gate, forget_gate, head_gain)
    part = jnp.dot(mixed_heads, w_out, preferred_element_type=f32).astype(bf16)
    side = lax.axis_index("tp")
    pairs = [(0, 1), (1, 0)]
    other = lax.dynamic_slice_in_dim(part, (1 - side) * own_rows, own_rows)
    kept = lax.dynamic_slice_in_dim(part, side * own_rows, own_rows)
    projected = kept.astype(f32) + lax.ppermute(other, "tp", pairs).astype(f32)
    updated = (residual.astype(f32) + projected).astype(bf16)
    updated_wide = updated.astype(f32)
    normed = (
        updated_wide
        * lax.rsqrt(jnp.mean(updated_wide * updated_wide, axis=-1, keepdims=True) + epsilon)
        * norm_gain
    ).astype(bf16)
    expert_count = lax.axis_size("sp") * lax.axis_size("tp")
    capacity = own_rows * routes.shape[1] * lax.axis_size("tp") // expert_count
    hit, weights = routing(routes, route_weight, expert_count, capacity)
    outgoing = lax.dot_general(
        hit, normed, (((0,), (0,)), ((), ())), preferred_element_type=f32
    ).astype(bf16)
    arrived = lax.all_to_all(
        outgoing.reshape(expert_count, capacity, model_width),
        ("sp", "tp"), split_axis=0, concat_axis=0, tiled=True,
    )
    shared = expert_layer(normed, shared_gate, shared_up, shared_down)
    answer = expert_layer(
        arrived.reshape(expert_count * capacity, model_width), w_gate[0], w_up[0], w_down[0]
    ).astype(bf16)
    returned = lax.all_to_all(
        answer.reshape(expert_count, capacity, model_width),
        ("sp", "tp"), split_axis=0, concat_axis=0, tiled=True,
    ).reshape(expert_count * capacity, model_width)
    high, low = two_parts(weights)
    routed = jnp.dot(high, returned, preferred_element_type=f32) + jnp.dot(
        low, returned, preferred_element_type=f32
    )
    return (updated_wide + shared + routed).astype(bf16)


def solution(mesh):
    return jax.shard_map(
        local,
        mesh=mesh,
        in_specs=(
            P(("sp", "tp"), None),
            P("sp", "tp"),
            P("sp", "tp"),
            P("sp", "tp"),
            P("sp", "tp"),
            P(None, "sp", "tp"),
            P(None, "sp", "tp"),
            P("tp"),
            P("tp", None),
            P(),
            P(),
            P(),
            P(),
            P(("sp", "tp"), None, None),
            P(("sp", "tp"), None, None),
            P(("sp", "tp"), None, None),
            P(("sp", "tp"), None),
            P(("sp", "tp"), None),
        ),
        out_specs=P(("sp", "tp"), None),
        check_vma=False,
    )
```
